32 devices in a mesh: st: 8 (over z, x), tp: 4 (over y, core).
Axes of the slice: x: 2, y: 2, z: 4, core: 2. Of those that a mesh axis runs over, the one named last changes fastest.
Arguments:
- tokens: bfloat16 [8192, 4096], P('st'), may hold values from -6 to 6
- passage_ids: int32 [128, 4], P('st'), may hold values from 0 to 23, as said below
- store: bfloat16 [24, 128, 4096], P('st'), may hold values from -6 to 6
- mix_gain: bfloat16 [4096], replicated, may hold values from 0.099609375 to 1.8984375
- w_query: bfloat16 [4096, 512], P(None, 'tp'), may hold values from -0.09375 to 0.09375
- w_key: bfloat16 [4096, 512], P(None, 'tp'), may hold values from -0.09375 to 0.09375
- w_value: bfloat16 [4096, 512], P(None, 'tp'), may hold values from -0.09375 to 0.09375
- w_cross_out: bfloat16 [512, 1024], P('tp'), may hold values from -0.5 to 0.5
- head_scale: float32 [4], replicated, may hold values from 1 to 4
- w_pool_in: bfloat16 [4096, 1024], P(None, 'tp'), may hold values from -0.09375 to 0.09375
- w_pool_mix: bfloat16 [4, 256, 256], replicated, may hold values from -0.375 to 0.375
- pool_scale: bfloat16 [1024], replicated, may hold values from 0.099609375 to 1.8984375
- gate_weight: float32 [1024], replicated, may hold values from -4 to 4
Outputs:
- mixed: bfloat16 [8192, 1024], P('st', 'tp')
The draws below stay inside these ranges and needn't reach their ends.
Inputs may be any that keep to these rules, and one draw needn't show every extreme that they name: `passage_ids`: passage p is held by index p // 3 of st. The 64 ids of one index of st (its aligned blocks of rows) fall on exactly 4 owners, 16 ids on each; one owner receives 16 ids from every index of st.
All inputs are finite; a program needn't handle non-finite values.
Results may differ from the reference program's by a relative error of at most 0.013.
Values may be sent and summed in bfloat16 or wider, within the bound.
A program may use at most 128 MiB of HBM per device.

```python
import math
import jax
import jax.numpy as jnp
from jax import lax

D = 4096
HEADS = 4
HEAD_DIM = 128
POOL_WIDTH = 1024
POOL_GROUPS = 4
GROUP_WIDTH = 256
SEQ_LEN = 128
BLOCK = 64
NPB = 4
P_LEN = 128
PASS_DEV = 3
TOKENS = 8192
BLOCKS = 128
PASSAGES = 24
REQ_DEV = 64
CAP = 16
N_ST = 8


def draw_passage_ids(key, part):
    hot_owner = jax.random.randint(jax.random.fold_in(key, 7), (), 0, N_ST)
    shifts = jnp.arange(N_ST).astype(jnp.int32)

    def one_device(device):
        device_key = jax.random.fold_in(key, device + 1000)
        priority = jax.random.randint(jax.random.fold_in(device_key, 1), (N_ST,), 0, 1 << 20) * N_ST + shifts
        priority = jnp.where(shifts == N_ST - 1, -3, priority)
        priority = jnp.where(shifts == N_ST // 2, jnp.minimum(priority, -2), priority)
        priority = jnp.where(shifts == (hot_owner - device) % N_ST, jnp.minimum(priority, -1), priority)
        ordering = jnp.argsort(priority, stable=True).astype(jnp.int32)
        owners = (device + ordering[jnp.arange(REQ_DEV) // CAP]) % N_ST
        first_pick = jax.random.randint(jax.random.fold_in(device_key, 2), (REQ_DEV,), 0, PASS_DEV)
        second_pick = jax.random.randint(jax.random.fold_in(device_key, 3), (REQ_DEV,), 0, PASS_DEV)
        chosen = owners * PASS_DEV + jnp.minimum(first_pick, second_pick)
        shuffle = jax.random.permutation(jax.random.fold_in(device_key, 4), REQ_DEV)
        return chosen[shuffle]
    all_ids = jax.vmap(one_device)(jnp.arange(N_ST).astype(jnp.int32))
    return all_ids.reshape(N_ST * REQ_DEV // NPB, NPB).astype(jnp.int32)


def shard_levels(rng, dims, pieces, low, largest):
    def one(axis_at, parts):
        heights = jax.random.uniform(jax.random.fold_in(jax.random.fold_in(rng, 6), axis_at), (parts,), jnp.float32, low / len(pieces), largest / len(pieces))
        return jnp.repeat(jnp.exp(heights), dims[axis_at] // parts).reshape((-1,) + (1,) * (len(dims) - axis_at - 1))

    level = one(*pieces[0])
    for cut in pieces[1:]:
        level = level * one(*cut)
    return level


def centred(rng, dims, spread, reach, split=(), kind=jnp.bfloat16):
    drawn = spread * jax.random.normal(rng, dims, jnp.float32)
    if split:
        drawn = drawn * shard_levels(rng, dims, split, -0.22, 0.18)
    return jnp.clip(drawn, -reach, reach).astype(kind)


def setup_inputs(seed: int = 0) -> dict:
    keys = jax.random.split(jax.random.key(seed), 14)
    return {
        "tokens": centred(keys[0], (TOKENS, D), 1.0, 6.0, ((0, 8),)),
        "passage_ids": draw_passage_ids(jax.random.fold_in(keys[13], 71), 0),
        "store": centred(keys[2], (PASSAGES, P_LEN, D), 1.0, 6.0, ((0, 8),)),
        "mix_gain": jnp.clip(1.0 + 0.18 * jax.random.normal(keys[3], (D,), jnp.float32), 0.099609375, 1.8984375).astype(jnp.bfloat16),
        "w_query": centred(keys[4], (D, HEADS * HEAD_DIM), D ** -0.5, 0.09375, ((1, 4),)),
        "w_key": centred(keys[5], (D, HEADS * HEAD_DIM), D ** -0.5, 0.09375, ((1, 4),)),
        "w_value": centred(keys[6], (D, HEADS * HEAD_DIM), D ** -0.5, 0.09375, ((1, 4),)),
        "w_cross_out": centred(keys[7], (HEADS * HEAD_DIM, POOL_WIDTH), HEAD_DIM ** -0.5, 0.5, ((0, 4),)),
        "head_scale": jnp.clip(jnp.exp(jax.random.uniform(keys[8], (HEADS,), jnp.float32, math.log(1.0), math.log(4.0))), 1.0, 4.0),
        "w_pool_in": centred(keys[9], (D, POOL_WIDTH), D ** -0.5, 0.09375, ((1, 4),)),
        "w_pool_mix": centred(keys[10], (POOL_GROUPS, GROUP_WIDTH, GROUP_WIDTH), GROUP_WIDTH ** -0.5, 0.375),
        "pool_scale": jnp.clip(1.0 + 0.18 * jax.random.normal(keys[11], (POOL_WIDTH,), jnp.float32), 0.099609375, 1.8984375).astype(jnp.bfloat16),
        "gate_weight": centred(keys[12], (POOL_WIDTH,), 1.0, 4.0, (), jnp.float32),
    }


EPSILON = 1e-06

def head_normalize(values):
    return values * lax.rsqrt(lax.optimization_barrier(jnp.mean(values * values, axis=-1, keepdims=True)) + EPSILON)

def normalize_rows(tokens, mix_gain):
    floats = tokens.astype(jnp.float32)
    scaled = floats * lax.rsqrt(lax.optimization_barrier(jnp.mean(floats * floats, axis=-1, keepdims=True)) + EPSILON)
    return (scaled * mix_gain.astype(jnp.float32)).astype(jnp.bfloat16)

def pool_residual(pooled_in, channel_ids):
    row_count, chan_width = pooled_in.shape
    sequences = pooled_in.astype(jnp.float32).reshape(row_count // SEQ_LEN, SEQ_LEN, chan_width)
    running = jnp.cumsum(sequences, axis=1)
    padded = jnp.concatenate([jnp.zeros((sequences.shape[0], 16, chan_width), jnp.float32), running], axis=1)
    upper_sum = padded[:, 16:]
    position = jnp.arange(SEQ_LEN).astype(jnp.int32)[None, :, None]
    result = jnp.zeros_like(sequences)
    for section_index in range(4):
        window = 2 << section_index
        lower_sum = padded[:, 16 - window:16 - window + SEQ_LEN]
        counted = jnp.minimum(position + 1, window).astype(jnp.float32)
        average = (upper_sum - lower_sum) / counted
        chosen = (channel_ids // GROUP_WIDTH == section_index)[None, None, :]
        result = jnp.where(chosen, average - sequences, result)
    return result.reshape(row_count, chan_width).astype(jnp.bfloat16)

def reference(tokens, passage_ids, store, mix_gain, w_query, w_key, w_value, w_cross_out, head_scale, w_pool_in, w_pool_mix, pool_scale, gate_weight):
    normed = normalize_rows(tokens, mix_gain)
    pooled_in = jnp.dot(normed, w_pool_in, preferred_element_type=jnp.float32).astype(jnp.bfloat16)
    residual = pool_residual(pooled_in, jnp.arange(POOL_WIDTH).astype(jnp.int32))
    grouped = residual.astype(jnp.float32).reshape(TOKENS, POOL_GROUPS, GROUP_WIDTH)
    pool_out = jnp.einsum('tgc,gce->tge', grouped, w_pool_mix.astype(jnp.float32)).reshape(TOKENS, POOL_WIDTH)
    pool_out = pool_out * pool_scale.astype(jnp.float32)
    queries = head_normalize(jnp.dot(normed, w_query, preferred_element_type=jnp.float32).reshape(TOKENS, HEADS, HEAD_DIM)).astype(jnp.bfloat16)
    flat_store = store.reshape(PASSAGES * P_LEN, D)
    passage_keys = head_normalize(jnp.dot(flat_store, w_key, preferred_element_type=jnp.float32).reshape(PASSAGES, P_LEN, HEADS, HEAD_DIM)).astype(jnp.bfloat16)
    passage_values = jnp.dot(flat_store, w_value, preferred_element_type=jnp.float32).astype(jnp.bfloat16).reshape(PASSAGES, P_LEN, HEADS, HEAD_DIM)
    scales = head_scale.astype(jnp.float32) / math.sqrt(HEAD_DIM)

    def one_block(inputs):
        block_queries, block_ids = inputs
        block_keys = passage_keys[block_ids].astype(jnp.float32)
        block_values = passage_values[block_ids].astype(jnp.float32)
        scores = jnp.einsum('qhd,jkhd->hqjk', block_queries.astype(jnp.float32), block_keys) * scales[:, None, None, None]
        weights = jnp.exp(scores)
        totals = lax.optimization_barrier(jnp.sum(weights, axis=(2, 3)))
        rounded = lax.optimization_barrier(weights.astype(jnp.bfloat16))
        partial_out = jnp.einsum('hqjk,jkhd->jqhd', rounded.astype(jnp.float32), block_values)
        partial_out = lax.optimization_barrier(partial_out.astype(jnp.bfloat16))
        summed = lax.optimization_barrier(jnp.sum(partial_out.astype(jnp.float32), axis=0))
        return (summed / jnp.transpose(totals)[:, :, None]).astype(jnp.bfloat16)
    attended = lax.map(one_block, (queries.reshape(BLOCKS, BLOCK, HEADS, HEAD_DIM), passage_ids))
    attended = attended.reshape(TOKENS, HEADS, HEAD_DIM)
    cross_sum = jnp.zeros((TOKENS, POOL_WIDTH), jnp.float32)
    for head_index in range(HEADS):
        rows_of_head = w_cross_out[head_index * HEAD_DIM:(head_index + 1) * HEAD_DIM]
        cross_term = jnp.dot(attended[:, head_index], rows_of_head, preferred_element_type=jnp.float32)
        cross_term = lax.optimization_barrier(cross_term.astype(jnp.bfloat16))
        cross_sum = cross_sum + cross_term.astype(jnp.float32)
    gate_value = jax.nn.sigmoid(pooled_in.astype(jnp.float32) * gate_weight.astype(jnp.float32))
    return (pool_out + gate_value * cross_sum).astype(jnp.bfloat16)
```

```python
import math

import jax
import jax.numpy as jnp
from jax import lax
from jax.sharding import PartitionSpec as P

HEAD_DIM = 128
GROUP_WIDTH = 256
SEQ_LEN = 128


EPSILON = 1e-06


def head_normalize(values):
    return values * lax.rsqrt(jnp.mean(values * values, axis=-1, keepdims=True) + EPSILON)


def pool_residual(pooled_in, channel_ids):
    row_count, chan_width = pooled_in.shape
    sequences = pooled_in.astype(jnp.float32).reshape(row_count // SEQ_LEN, SEQ_LEN, chan_width)
    running = jnp.cumsum(sequences, axis=1)
    padded = jnp.concatenate(
        [jnp.zeros((sequences.shape[0], 16, chan_width), jnp.float32), running], axis=1
    )
    upper_sum = padded[:, 16:]
    position = jnp.arange(SEQ_LEN)[None, :, None]
    result = jnp.zeros_like(sequences)
    for section_index in range(4):
        window = 2 << section_index
        lower_sum = padded[:, 16 - window : 16 - window + SEQ_LEN]
        counted = jnp.minimum(position + 1, window).astype(jnp.float32)
        average = (upper_sum - lower_sum) / counted
        chosen = (channel_ids // GROUP_WIDTH == section_index)[None, None, :]
        result = jnp.where(chosen, average - sequences, result)
    return result.reshape(row_count, chan_width).astype(jnp.bfloat16)


def per_device(
    tokens,
    passage_ids,
    store,
    mix_gain,
    w_query,
    w_key,
    w_value,
    w_cross_out,
    head_scale,
    w_pool_in,
    w_pool_mix,
    pool_scale,
    gate_weight,
):
    row_count = tokens.shape[0]
    floats = tokens.astype(jnp.float32)
    scaled = floats * lax.rsqrt(jnp.mean(floats * floats, axis=-1, keepdims=True) + EPSILON)
    normed = (scaled * mix_gain.astype(jnp.float32)).astype(jnp.bfloat16)
    pooled_in = jnp.dot(normed, w_pool_in, preferred_element_type=jnp.float32).astype(jnp.bfloat16)
    local_width = pooled_in.shape[1]
    tensor_rank = lax.axis_index("tp")
    offset = tensor_rank * local_width
    residual = pool_residual(pooled_in, offset + jnp.arange(local_width))
    local_groups = local_width // GROUP_WIDTH
    mix_local = lax.dynamic_slice_in_dim(w_pool_mix, tensor_rank * local_groups, local_groups, 0)
    pool_out = jnp.einsum(
        "tgc,gce->tge",
        residual.reshape(row_count, local_groups, GROUP_WIDTH),
        mix_local,
        preferred_element_type=jnp.float32,
    )
    pool_out = pool_out.reshape(row_count, local_width) * lax.dynamic_slice_in_dim(
        pool_scale, offset, local_width
    ).astype(jnp.float32)
    gate_value = jax.nn.sigmoid(
        pooled_in.astype(jnp.float32) * lax.dynamic_slice_in_dim(gate_weight, offset, local_width)
    )
    heads_local = w_query.shape[1] // HEAD_DIM
    scales = lax.dynamic_slice_in_dim(
        head_scale, tensor_rank * heads_local, heads_local
    ) / math.sqrt(HEAD_DIM)
    queries = head_normalize(
        jnp.dot(normed, w_query, preferred_element_type=jnp.float32).reshape(
            row_count, heads_local, HEAD_DIM
        )
    ).astype(jnp.bfloat16)
    owned_count, passage_len = (store.shape[0], store.shape[1])
    flat_store = store.reshape(owned_count * passage_len, store.shape[2])
    keys_own = head_normalize(
        jnp.dot(flat_store, w_key, preferred_element_type=jnp.float32).reshape(
            owned_count, passage_len, heads_local, HEAD_DIM
        )
    ).astype(jnp.bfloat16)
    values_own = (
        jnp.dot(flat_store, w_value, preferred_element_type=jnp.float32)
        .astype(jnp.bfloat16)
        .reshape(owned_count, passage_len, heads_local, HEAD_DIM)
    )
    block_count, per_block = passage_ids.shape
    block_rows = row_count // block_count
    pair_own = jnp.concatenate([keys_own, values_own], axis=-1)
    pair_all = lax.all_gather(pair_own, "st", axis=0, tiled=True)
    chosen = pair_all[passage_ids.reshape(-1)].reshape(
        block_count, per_block * passage_len, heads_local, 2 * HEAD_DIM
    )
    block_queries = queries.reshape(block_count, block_rows, heads_local, HEAD_DIM)
    scores = (
        jnp.einsum(
            "bqhd,bkhd->bhqk",
            block_queries,
            chosen[..., :HEAD_DIM],
            preferred_element_type=jnp.float32,
        )
        * scales[None, :, None, None]
    )
    weights = jnp.exp(scores)
    totals = jnp.transpose(jnp.sum(weights, axis=3), (0, 2, 1))
    summed = jnp.einsum(
        "bhqk,bkhd->bqhd",
        weights.astype(jnp.bfloat16),
        chosen[..., HEAD_DIM:],
        preferred_element_type=jnp.float32,
    )
    attended = (
        (summed / totals[..., None]).astype(jnp.bfloat16).reshape(row_count, heads_local * HEAD_DIM)
    )
    cross_columns = lax.all_to_all(w_cross_out, "tp", split_axis=1, concat_axis=0, tiled=True)
    attended_all = lax.all_gather(attended, "tp", axis=1, tiled=True)
    cross_sum = jnp.dot(attended_all, cross_columns, preferred_element_type=jnp.float32)
    return (pool_out + gate_value * cross_sum).astype(jnp.bfloat16)


def solution(mesh):
    return jax.shard_map(
        per_device,
        mesh=mesh,
        in_specs=(
            P("st", None),
            P("st", None),
            P("st", None, None),
            P(),
            P(None, "tp"),
            P(None, "tp"),
            P(None, "tp"),
            P("tp", None),
            P(),
            P(None, "tp"),
            P(),
            P(),
            P(),
        ),
        out_specs=P("st", "tp"),
        check_vma=False,
    )
```

```python
import functools
import math

import jax
import jax.numpy as jnp
from jax import lax
from jax.experimental import pallas as pl
from jax.experimental.pallas import tpu as pltpu
from jax.sharding import PartitionSpec as P

MESH = pl.DeviceIdType.MESH
SEQ_LEN = 128
EPSILON = 1e-06
TILE = 256
F32 = jnp.float32
BF16 = jnp.bfloat16


def kernel(
    n,
    tp_size,
    tok_h,
    ids_s,
    store_h,
    gain_v,
    wq_h,
    wk_h,
    wv_h,
    wc_h,
    hs_s,
    wp_h,
    mix_h,
    ps_v,
    gw_v,
    out_v,
    tok,
    store,
    wkv,
    wqp,
    mix,
    wc,
    kv,
    xg,
    rs,
    q,
    pool,
    gate,
    num,
    tot,
    att,
    local_sem,
    tok_sem,
    store_sem,
    wc_send,
    wc_recv,
    kv_send,
    kv_recv,
    att_send,
    att_recv,
    *,
    hd,
):
    st = lax.axis_index("st")
    tp = lax.axis_index("tp")
    half_n = n // 2
    owned, p_len, depth = store.shape
    rows = tok.shape[0]
    tiles = rows // TILE
    width = mix.shape[0]
    blocks, per_block = ids_s.shape
    block_rows = rows // blocks
    tile_blocks = TILE // block_rows
    half_rows = p_len // 2

    pos = jnp.where(lax.rem(st, 2) == 0, st // 2, n - 1 - st // 2)

    def ring_id(p):
        p = lax.rem(p + 2 * n, n)
        return jnp.where(p < half_n, 2 * p, 2 * (n - 1 - p) + 1)

    right = {"st": ring_id(pos + 1)}
    left = {"st": ring_id(pos - 1)}
    core_mate = tp + 1 - 2 * lax.rem(tp, 2)
    far_mate = lax.rem(tp + 2, tp_size)
    far_core = lax.rem(core_mate + 2, tp_size)

    barrier = pltpu.get_barrier_semaphore()
    for target in (right, left, {"tp": core_mate}, {"tp": far_mate}, {"tp": far_core}):
        pl.semaphore_signal(barrier, inc=1, device_id=target, device_id_type=MESH)

    wk_copy = pltpu.make_async_copy(wk_h, wkv.at[:, 0:hd], local_sem.at[0])
    wv_copy = pltpu.make_async_copy(wv_h, wkv.at[:, hd : 2 * hd], local_sem.at[1])
    wk_copy.start()
    wv_copy.start()
    store_copies = [
        pltpu.make_async_copy(store_h.at[i], store.at[i], store_sem.at[i]) for i in range(owned)
    ]
    for copy in store_copies:
        copy.start()
    wq_copy = pltpu.make_async_copy(wq_h, wqp.at[:, 0:hd], local_sem.at[2])
    wp_copy = pltpu.make_async_copy(wp_h, wqp.at[:, hd : hd + width], local_sem.at[3])
    mix_copy = pltpu.make_async_copy(mix_h.at[tp], mix, local_sem.at[4])
    wq_copy.start()
    wp_copy.start()

    def tok_copy(t):
        part = pl.ds(pl.multiple_of(t * TILE, TILE), TILE)
        return pltpu.make_async_copy(tok_h.at[part], tok.at[part], tok_sem.at[t])

    for t in range(tiles):
        tok_copy(t).start()
    mix_copy.start()

    def columns_of(index):
        return wc_h.at[:, pl.ds(pl.multiple_of(index * width, width), width)]

    wc_copy = pltpu.make_async_copy(columns_of(tp), wc.at[tp], local_sem.at[5])
    wc_copy.start()

    def wc_remote(k, mate, slot):
        return pltpu.make_async_remote_copy(
            src_ref=columns_of(mate),
            dst_ref=wc.at[slot],
            send_sem=wc_send.at[k],
            recv_sem=wc_recv.at[k],
            device_id={"tp": mate},
            device_id_type=MESH,
        )

    mates = (core_mate, far_mate, far_core)

    def piece(way, step, i, half):
        origin = ring_id(pos - (step - 1)) if way == 0 else ring_id(pos + (step - 1))
        ref = kv.at[origin, i]
        if half:
            ref = kv.at[origin, i, pl.ds(way * half_rows, half_rows)]
        return pltpu.make_async_remote_copy(
            src_ref=ref,
            dst_ref=ref,
            send_sem=kv_send.at[way, step - 1, i],
            recv_sem=kv_recv.at[way, step - 1, i],
            device_id=right if way == 0 else left,
            device_id_type=MESH,
        )

    def arrived(way, step, i, half):
        origin = ring_id(pos - step) if way == 0 else ring_id(pos + step)
        ref = kv.at[origin, i]
        if half:
            ref = kv.at[origin, i, pl.ds(way * half_rows, half_rows)]
        pltpu.make_async_remote_copy(
            src_ref=ref,
            dst_ref=ref,
            send_sem=kv_send.at[way, step - 1, i],
            recv_sem=kv_recv.at[way, step - 1, i],
            device_id=right if way == 0 else left,
            device_id_type=MESH,
        ).wait_recv()

    def head_normal(values):
        return values * lax.rsqrt(jnp.mean(values * values, axis=-1, keepdims=True) + EPSILON)

    wk_copy.wait()
    wv_copy.wait()
    for i in range(owned):
        store_copies[i].wait()
        both = jnp.dot(store[i], wkv[...], preferred_element_type=F32)
        kv[st, i, :, 0:hd] = head_normal(both[:, 0:hd]).astype(BF16)
        kv[st, i, :, hd : 2 * hd] = both[:, hd : 2 * hd].astype(BF16)
        if i == 0:
            pl.semaphore_wait(barrier, 5)
        piece(0, 1, i, False).start()
        piece(1, 1, i, False).start()
    for k in range(3):
        wc_remote(k, mates[k], tp).start()

    def tick(step, i, forward_half):
        for way in (0, 1):
            arrived(way, step, i, False)
            piece(way, step + 1, i, forward_half).start()

    wq_copy.wait()
    wp_copy.wait()
    mix_copy.wait()
    window = jnp.left_shift(2, tp)
    row_at = lax.broadcasted_iota(jnp.int32, (SEQ_LEN, SEQ_LEN), 0)
    col_at = lax.broadcasted_iota(jnp.int32, (SEQ_LEN, SEQ_LEN), 1)
    gap = row_at - col_at
    band = jnp.where((gap >= 0) & (gap < window), 1.0, 0.0).astype(BF16)
    position = lax.broadcasted_iota(jnp.int32, (SEQ_LEN, width), 0)
    counted = jnp.minimum(position + 1, window).astype(F32)
    strip = 32

    def token_tile(t, carry):
        tok_copy(t).wait()

        def norm_strip(u, carry):
            inner = pl.ds(pl.multiple_of(u * strip, strip), strip)
            x = tok[pl.ds(pl.multiple_of(t * TILE + u * strip, strip), strip), :]
            xf = x.astype(F32)
            square = jnp.mean(xf * xf, axis=-1, keepdims=True)
            rs[inner, :] = jnp.broadcast_to(lax.rsqrt(square + EPSILON), (strip, 128))
            xg[inner, :] = (xf * gain_v[...]).astype(BF16)
            return carry

        lax.fori_loop(0, TILE // strip, norm_strip, 0)
        part = pl.ds(pl.multiple_of(t * TILE, TILE), TILE)
        scale_row = rs[:, 0:1]
        projected = jnp.dot(xg[...], wqp[...], preferred_element_type=F32) * scale_row
        q[part, :] = head_normal(projected[:, 0:hd]).astype(BF16)
        pooled = projected[:, hd : hd + width].astype(BF16)
        for sequence in range(TILE // SEQ_LEN):
            part_in = pooled[sequence * SEQ_LEN : (sequence + 1) * SEQ_LEN]
            values = part_in.astype(F32)
            sums = jnp.dot(band, part_in, preferred_element_type=F32)
            residual = (sums / counted - values).astype(BF16)
            place = pl.ds(
                pl.multiple_of(t * TILE + sequence * SEQ_LEN, SEQ_LEN), SEQ_LEN
            )
            mixed = jnp.dot(residual, mix[...], preferred_element_type=F32)
            pool[place, :] = mixed * ps_v[tp].astype(F32)
            gate[place, :] = jax.nn.sigmoid(values * gw_v[tp])
        num[part, :] = jnp.zeros((TILE, hd), F32)
        tot[part, :] = jnp.zeros((TILE, p_len), F32)

        @pl.when(t >= tiles - owned)
        def _():
            tick(1, t - (tiles - owned), False)

        return carry

    lax.fori_loop(0, tiles, token_tile, 0)

    head_factor = hs_s[tp] / math.sqrt(hd)

    def attend(t, sources):
        part = pl.ds(pl.multiple_of(t * TILE, TILE), TILE)
        keys = jnp.concatenate([kv[o, i, :, 0:hd] for o, i in sources], axis=0)
        vals = jnp.concatenate([kv[o, i, :, hd : 2 * hd] for o, i in sources], axis=0)
        scores = lax.dot_general(
            q[part, :], keys, (((1,), (1,)), ((), ())), preferred_element_type=F32
        )
        weights = jnp.exp(scores * head_factor)
        parts = []
        total = None
        for k, (o, i) in enumerate(sources):
            wanted = o * owned + i
            bands = []
            for b in range(tile_blocks):
                count = jnp.int32(0)
                for j in range(per_block):
                    apart = ids_s[t * tile_blocks + b, j] - wanted
                    count = count + 1 - jnp.minimum(jnp.abs(apart), 1)
                piece_w = weights[
                    b * block_rows : (b + 1) * block_rows, k * p_len : (k + 1) * p_len
                ]
                bands.append(piece_w * count.astype(F32))
            chunk = jnp.concatenate(bands, axis=0)
            total = chunk if total is None else total + chunk
            parts.append(chunk.astype(BF16))
        flat = jnp.concatenate(parts, axis=1)
        return part, jnp.dot(flat, vals, preferred_element_type=F32), total

    def attend_all(sources):
        def one(t, carry):
            part, numer, total = attend(t, sources)
            num[part, :] = num[part, :] + numer
            tot[part, :] = tot[part, :] + total
            return carry

        lax.fori_loop(0, tiles, one, 0)

    def both_sides(step, i):
        return [(ring_id(pos - step), i), (ring_id(pos + step), i)]

    attend_all([(st, i) for i in range(owned)])

    def full_step(step, carry):
        for i in range(owned):
            tick(step, i, False)
            attend_all(both_sides(step - 1, i))
        return carry

    lax.fori_loop(2, half_n - 1, full_step, 0)
    for i in range(owned):
        tick(half_n - 1, i, True)
        attend_all(both_sides(half_n - 2, i))
    for i in range(owned):
        attend_all(both_sides(half_n - 1, i))
    for i in range(owned):
        arrived(0, half_n, i, True)
        arrived(1, half_n, i, True)

    def att_remote(k, t, mate, slot):
        ref = att.at[slot, pl.ds(pl.multiple_of(t * TILE, TILE), TILE)]
        return pltpu.make_async_remote_copy(
            src_ref=ref,
            dst_ref=ref,
            send_sem=att_send.at[k, t],
            recv_sem=att_recv.at[k, t],
            device_id={"tp": mate},
            device_id_type=MESH,
        )

    opposite = ring_id(pos + half_n)

    def last_tile(t, carry):
        part, numer, total = attend(t, [(opposite, i) for i in range(owned)])
        below = jnp.sum(tot[part, :] + total, axis=-1, keepdims=True)
        att[tp, part, :] = ((num[part, :] + numer) / below).astype(BF16)
        att_remote(0, t, far_mate, tp).start()
        att_remote(1, t, core_mate, tp).start()
        return carry

    lax.fori_loop(0, tiles, last_tile, 0)

    wc_copy.wait()
    for k in range(3):
        wc_remote(k, mates[k], mates[k]).wait_recv()

    def finish(t):
        att_remote(1, t, core_mate, core_mate).wait_recv()
        att_remote(2, t, core_mate, far_core).wait_recv()
        part = pl.ds(pl.multiple_of(t * TILE, TILE), TILE)
        cross = None
        for h in range(tp_size):
            term = jnp.dot(att[h, part, :], wc[h], preferred_element_type=F32)
            cross = term if cross is None else cross + term
        out_v[part, :] = (pool[part, :] + gate[part, :] * cross).astype(BF16)

    def exchange(t, carry):
        att_remote(0, t, far_mate, far_mate).wait_recv()
        att_remote(2, t, core_mate, far_mate).start()

        @pl.when(t > 0)
        def _():
            finish(t - 1)

        return carry

    lax.fori_loop(0, tiles, exchange, 0)
    finish(tiles - 1)

    for k in range(3):
        wc_remote(k, mates[k], tp).wait_send()

    def sent(step, carry):
        for i in range(owned):
            piece(0, step, i, False).wait_send()
            piece(1, step, i, False).wait_send()
        return carry

    lax.fori_loop(1, half_n, sent, 0)
    for i in range(owned):
        piece(0, half_n, i, True).wait_send()
        piece(1, half_n, i, True).wait_send()
    for t in range(tiles):
        att_remote(0, t, far_mate, tp).wait_send()
        att_remote(1, t, core_mate, tp).wait_send()
        att_remote(2, t, core_mate, far_mate).wait_send()


def solution(mesh):
    n = mesh.shape["st"]
    tp_size = mesh.shape["tp"]

    def per_device(
        tokens,
        passage_ids,
        store,
        mix_gain,
        w_query,
        w_key,
        w_value,
        w_cross_out,
        head_scale,
        w_pool_in,
        w_pool_mix,
        pool_scale,
        gate_weight,
    ):
        rows, depth = tokens.shape
        owned, p_len, _ = store.shape
        hd = w_query.shape[1]
        width = w_pool_in.shape[1]
        tiles = rows // TILE
        half_n = n // 2
        hbm = pl.BlockSpec(memory_space=pl.ANY)
        vmem = pl.BlockSpec(memory_space=pltpu.VMEM)
        smem = pl.BlockSpec(memory_space=pltpu.SMEM)
        dma = pltpu.SemaphoreType.DMA
        return pl.pallas_call(
            functools.partial(kernel, n, tp_size, hd=hd),
            out_shape=jax.ShapeDtypeStruct((rows, width), BF16),
            in_specs=[hbm, smem, hbm, vmem, hbm, hbm, hbm, hbm, smem, hbm, hbm, vmem, vmem],
            out_specs=vmem,
            scratch_shapes=[
                pltpu.VMEM((rows, depth), BF16),
                pltpu.VMEM((owned, p_len, depth), BF16),
                pltpu.VMEM((depth, 2 * hd), BF16),
                pltpu.VMEM((depth, hd + width), BF16),
                pltpu.VMEM((width, width), BF16),
                pltpu.VMEM((tp_size, hd, width), BF16),
                pltpu.VMEM((n, owned, p_len, 2 * hd), BF16),
                pltpu.VMEM((TILE, depth), BF16),
                pltpu.VMEM((TILE, 128), F32),
                pltpu.VMEM((rows, hd), BF16),
                pltpu.VMEM((rows, width), F32),
                pltpu.VMEM((rows, width), F32),
                pltpu.VMEM((rows, hd), F32),
                pltpu.VMEM((rows, p_len), F32),
                pltpu.VMEM((tp_size, rows, hd), BF16),
                dma((6,)),
                dma((tiles,)),
                dma((owned,)),
                dma((3,)),
                dma((3,)),
                dma((2, half_n, owned)),
                dma((2, half_n, owned)),
                dma((3, tiles)),
                dma((3, tiles)),
            ],
            compiler_params=pltpu.CompilerParams(
                collective_id=0,
                has_side_effects=True,
                vmem_limit_bytes=60 * 1024 * 1024,
            ),
        )(
            tokens,
            passage_ids,
            store,
            mix_gain.reshape(1, depth),
            w_query,
            w_key,
            w_value,
            w_cross_out,
            head_scale,
            w_pool_in,
            w_pool_mix,
            pool_scale.reshape(tp_size, 1, width),
            gate_weight.reshape(tp_size, 1, width),
        )

    return jax.shard_map(
        per_device,
        mesh=mesh,
        in_specs=(
            P("st", None),
            P("st", None),
            P("st", None, None),
            P(),
            P(None, "tp"),
            P(None, "tp"),
            P(None, "tp"),
            P("tp", None),
            P(),
            P(None, "tp"),
            P(),
            P(),
            P(),
        ),
        out_specs=P("st", "tp"),
        check_vma=False,
    )
```

```python
import functools
import math

import jax
import jax.numpy as jnp
from jax import lax
from jax.experimental import pallas as pl
from jax.experimental.pallas import tpu as pltpu
from jax.sharding import PartitionSpec as P

MESH = pl.DeviceIdType.MESH
SEQ_LEN = 128
EPSILON = 1e-06
TILE = 256
F32 = jnp.float32
BF16 = jnp.bfloat16


def kernel(
    n,
    tp_size,
    tok_h,
    ids_s,
    store_h,
    gain_v,
    wq_h,
    wk_h,
    wv_h,
    wc_h,
    hs_s,
    wp_h,
    mix_h,
    ps_v,
    gw_v,
    out_v,
    tok,
    store,
    wk,
    wv,
    wq,
    wp,
    gain_b,
    mix,
    wc,
    kv,
    q,
    pool,
    gate,
    num,
    tot,
    att,
    local_sem,
    tok_sem,
    store_sem,
    wc_send,
    wc_recv,
    kv_send,
    kv_recv,
    att_send,
    att_recv,
    *,
    hd,
):
    st = lax.axis_index("st")
    tp = lax.axis_index("tp")
    half_n = n // 2
    owned, p_len, depth = store.shape
    rows = tok.shape[0]
    tiles = rows // TILE
    width = mix.shape[0]
    per_block, blocks = ids_s.shape
    block_rows = rows // blocks
    tile_blocks = TILE // block_rows
    half_rows = p_len // 2

    pos = jnp.where(lax.rem(st, 2) == 0, st // 2, n - 1 - st // 2)

    def ring_id(p):
        p = lax.rem(p + 2 * n, n)
        return jnp.where(p < half_n, 2 * p, 2 * (n - 1 - p) + 1)

    right = {"st": ring_id(pos + 1)}
    left = {"st": ring_id(pos - 1)}
    core_mate = tp + 1 - 2 * lax.rem(tp, 2)
    far_mate = lax.rem(tp + 2, tp_size)
    far_core = lax.rem(core_mate + 2, tp_size)

    barrier = pltpu.get_barrier_semaphore()
    for target in (right, left, {"tp": core_mate}, {"tp": far_mate}, {"tp": far_core}):
        pl.semaphore_signal(barrier, inc=1, device_id=target, device_id_type=MESH)

    wk_copy = pltpu.make_async_copy(wk_h, wk, local_sem.at[0])
    wv_copy = pltpu.make_async_copy(wv_h, wv, local_sem.at[1])
    wk_copy.start()
    wv_copy.start()
    store_copies = [
        pltpu.make_async_copy(store_h.at[i], store.at[i], store_sem.at[i]) for i in range(owned)
    ]
    for copy in store_copies:
        copy.start()
    wq_copy = pltpu.make_async_copy(wq_h, wq, local_sem.at[2])
    wp_copy = pltpu.make_async_copy(wp_h, wp, local_sem.at[3])
    mix_copy = pltpu.make_async_copy(mix_h.at[tp], mix, local_sem.at[4])
    wq_copy.start()
    wp_copy.start()

    def tok_copy(t):
        part = pl.ds(pl.multiple_of(t * TILE, TILE), TILE)
        return pltpu.make_async_copy(tok_h.at[part], tok.at[part], tok_sem.at[t])

    for t in range(tiles):
        tok_copy(t).start()
    mix_copy.start()

    def columns_of(index):
        return wc_h.at[:, pl.ds(pl.multiple_of(index * width, width), width)]

    wc_copy = pltpu.make_async_copy(columns_of(tp), wc.at[tp], local_sem.at[5])
    wc_copy.start()

    def wc_remote(k, mate, slot):
        return pltpu.make_async_remote_copy(
            src_ref=columns_of(mate),
            dst_ref=wc.at[slot],
            send_sem=wc_send.at[k],
            recv_sem=wc_recv.at[k],
            device_id={"tp": mate},
            device_id_type=MESH,
        )

    mates = (core_mate, far_mate, far_core)

    def piece(way, step, i, half):
        origin = ring_id(pos - (step - 1)) if way == 0 else ring_id(pos + (step - 1))
        ref = kv.at[origin, i]
        if half:
            ref = kv.at[origin, i, pl.ds(way * half_rows, half_rows)]
        return pltpu.make_async_remote_copy(
            src_ref=ref,
            dst_ref=ref,
            send_sem=kv_send.at[way, step - 1, i],
            recv_sem=kv_recv.at[way, step - 1, i],
            device_id=right if way == 0 else left,
            device_id_type=MESH,
        )

    def arrived(way, step, i, half):
        origin = ring_id(pos - step) if way == 0 else ring_id(pos + step)
        ref = kv.at[origin, i]
        if half:
            ref = kv.at[origin, i, pl.ds(way * half_rows, half_rows)]
        pltpu.make_async_remote_copy(
            src_ref=ref,
            dst_ref=ref,
            send_sem=kv_send.at[way, step - 1, i],
            recv_sem=kv_recv.at[way, step - 1, i],
            device_id=right if way == 0 else left,
            device_id_type=MESH,
        ).wait_recv()

    def head_normal(values):
        return values * lax.rsqrt(jnp.mean(values * values, axis=-1, keepdims=True) + EPSILON)

    gain_b[...] = jnp.broadcast_to(gain_v[...].reshape(1, depth), (TILE, depth))
    wk_copy.wait()
    wv_copy.wait()
    for i in range(owned):
        store_copies[i].wait()
        pair = jnp.concatenate([wk[...], wv[...]], axis=1)
        both = jnp.dot(store[i], pair, preferred_element_type=F32)
        kv[st, i, :, 0:hd] = head_normal(both[:, 0:hd]).astype(BF16)
        kv[st, i, :, hd : 2 * hd] = both[:, hd : 2 * hd].astype(BF16)
        if i == 0:
            pl.semaphore_wait(barrier, 5)
        piece(0, 1, i, False).start()
        piece(1, 1, i, False).start()
    for k in range(3):
        wc_remote(k, mates[k], tp).start()

    def tick(step, i, forward_half):
        for way in (0, 1):
            arrived(way, step, i, False)
            piece(way, step + 1, i, forward_half).start()

    wq_copy.wait()
    wp_copy.wait()
    mix_copy.wait()
    window = jnp.left_shift(2, tp)
    row_at = lax.broadcasted_iota(jnp.int32, (SEQ_LEN, SEQ_LEN), 0)
    col_at = lax.broadcasted_iota(jnp.int32, (SEQ_LEN, SEQ_LEN), 1)
    gap = row_at - col_at
    band = jnp.where((gap >= 0) & (gap < window), 1.0, 0.0).astype(BF16)
    position = lax.broadcasted_iota(jnp.int32, (SEQ_LEN, width), 0)
    counted = jnp.minimum(position + 1, window).astype(F32)
    chunk = 1024
    scale_all = ps_v[...].astype(F32).reshape(1, tp_size * width)
    pool_row = scale_all[:, 0:width]
    for g in range(1, tp_size):
        pool_row = jnp.where(tp == g, scale_all[:, g * width : (g + 1) * width], pool_row)

    def token_tile(t, carry):
        tok_copy(t).wait()

        part = pl.ds(pl.multiple_of(t * TILE, TILE), TILE)
        projected = jnp.zeros((TILE, hd + width), F32)
        squares = jnp.zeros((TILE, 128), F32)
        for c in range(depth // chunk):
            cols = slice(c * chunk, (c + 1) * chunk)
            x = tok[part, cols]
            xf = x.astype(F32)
            xx = xf * xf
            for k in range(chunk // 128):
                squares = squares + xx[:, k * 128 : (k + 1) * 128]
            pair = jnp.concatenate([wq[cols, :], wp[cols, :]], axis=1)
            projected = projected + jnp.dot(
                x * gain_b[:, cols], pair, preferred_element_type=F32
            )
        mean_square = jnp.sum(squares, axis=-1, keepdims=True) / depth
        projected = projected * lax.rsqrt(mean_square + EPSILON)
        q[part, :] = head_normal(projected[:, 0:hd]).astype(BF16)
        pooled = projected[:, hd : hd + width].astype(BF16)
        for sequence in range(TILE // SEQ_LEN):
            part_in = pooled[sequence * SEQ_LEN : (sequence + 1) * SEQ_LEN]
            values = part_in.astype(F32)
            sums = jnp.dot(band, part_in, preferred_element_type=F32)
            residual = (sums / counted - values).astype(BF16)
            place = pl.ds(
                pl.multiple_of(t * TILE + sequence * SEQ_LEN, SEQ_LEN), SEQ_LEN
            )
            mixed = jnp.dot(residual, mix[...], preferred_element_type=F32)
            pool[place, :] = mixed * pool_row
            gate[place, :] = jax.nn.sigmoid(values * gw_v[tp])
        num[part, :] = jnp.zeros((TILE, hd), F32)
        tot[part, :] = jnp.zeros((TILE, p_len), F32)

        @pl.when(t >= tiles - owned)
        def _():
            tick(1, t - (tiles - owned), False)

        return carry

    lax.fori_loop(0, tiles, token_tile, 0)

    head_factor = hs_s[tp] / math.sqrt(hd)

    def attend(t, sources):
        part = pl.ds(pl.multiple_of(t * TILE, TILE), TILE)
        keys = jnp.concatenate([kv[o, i, :, 0:hd] for o, i in sources], axis=0)
        vals = jnp.concatenate([kv[o, i, :, hd : 2 * hd] for o, i in sources], axis=0)
        scores = lax.dot_general(
            q[part, :], keys, (((1,), (1,)), ((), ())), preferred_element_type=F32
        )
        weights = jnp.exp(scores * head_factor)
        parts = []
        total = None
        for k, (o, i) in enumerate(sources):
            wanted = o * owned + i
            bands = []
            for b in range(tile_blocks):
                count = jnp.int32(0)
                for j in range(per_block):
                    apart = ids_s[j, t * tile_blocks + b] - wanted
                    count = count + 1 - jnp.minimum(jnp.abs(apart), 1)
                piece_w = weights[
                    b * block_rows : (b + 1) * block_rows, k * p_len : (k + 1) * p_len
                ]
                bands.append(piece_w * count.astype(F32))
            chunk = jnp.concatenate(bands, axis=0)
            total = chunk if total is None else total + chunk
            parts.append(chunk.astype(BF16))
        flat = jnp.concatenate(parts, axis=1)
        return part, jnp.dot(flat, vals, preferred_element_type=F32), total

    def attend_all(sources):
        def one(t, carry):
            part, numer, total = attend(t, sources)
            num[part, :] = num[part, :] + numer
            tot[part, :] = tot[part, :] + total
            return carry

        lax.fori_loop(0, tiles, one, 0)

    def both_sides(step, i):
        return [(ring_id(pos - step), i), (ring_id(pos + step), i)]

    attend_all([(st, i) for i in range(owned)])

    def full_step(step, carry):
        for i in range(owned):
            tick(step, i, False)
            attend_all(both_sides(step - 1, i))
        return carry

    lax.fori_loop(2, half_n - 1, full_step, 0)
    for i in range(owned):
        tick(half_n - 1, i, True)
        attend_all(both_sides(half_n - 2, i))
    for i in range(owned):
        attend_all(both_sides(half_n - 1, i))
    for i in range(owned):
        arrived(0, half_n, i, True)
        arrived(1, half_n, i, True)

    def att_remote(k, t, mate, slot):
        ref = att.at[slot, pl.ds(pl.multiple_of(t * TILE, TILE), TILE)]
        return pltpu.make_async_remote_copy(
            src_ref=ref,
            dst_ref=ref,
            send_sem=att_send.at[k, t],
            recv_sem=att_recv.at[k, t],
            device_id={"tp": mate},
            device_id_type=MESH,
        )

    opposite = ring_id(pos + half_n)

    def last_tile(t, carry):
        part, numer, total = attend(t, [(opposite, i) for i in range(owned)])
        below = jnp.sum(tot[part, :] + total, axis=-1, keepdims=True)
        att[tp, part, :] = ((num[part, :] + numer) / below).astype(BF16)
        att_remote(0, t, far_mate, tp).start()
        att_remote(1, t, core_mate, tp).start()
        return carry

    lax.fori_loop(0, tiles, last_tile, 0)

    wc_copy.wait()
    for k in range(3):
        wc_remote(k, mates[k], mates[k]).wait_recv()

    def finish(t):
        att_remote(1, t, core_mate, core_mate).wait_recv()
        att_remote(2, t, core_mate, far_core).wait_recv()
        part = pl.ds(pl.multiple_of(t * TILE, TILE), TILE)
        cross = None
        for h in range(tp_size):
            term = jnp.dot(att[h, part, :], wc[h], preferred_element_type=F32)
            cross = term if cross is None else cross + term
        out_v[part, :] = (pool[part, :] + gate[part, :] * cross).astype(BF16)

    def exchange(t, carry):
        att_remote(0, t, far_mate, far_mate).wait_recv()
        att_remote(2, t, core_mate, far_mate).start()

        @pl.when(t > 0)
        def _():
            finish(t - 1)

        return carry

    lax.fori_loop(0, tiles, exchange, 0)
    finish(tiles - 1)

    for k in range(3):
        wc_remote(k, mates[k], tp).wait_send()

    def sent(step, carry):
        for i in range(owned):
            piece(0, step, i, False).wait_send()
            piece(1, step, i, False).wait_send()
        return carry

    lax.fori_loop(1, half_n, sent, 0)
    for i in range(owned):
        piece(0, half_n, i, True).wait_send()
        piece(1, half_n, i, True).wait_send()
    for t in range(tiles):
        att_remote(0, t, far_mate, tp).wait_send()
        att_remote(1, t, core_mate, tp).wait_send()
        att_remote(2, t, core_mate, far_mate).wait_send()


def solution(mesh):
    n = mesh.shape["st"]
    tp_size = mesh.shape["tp"]

    def per_device(
        tokens,
        passage_ids,
        store,
        mix_gain,
        w_query,
        w_key,
        w_value,
        w_cross_out,
        head_scale,
        w_pool_in,
        w_pool_mix,
        pool_scale,
        gate_weight,
    ):
        rows, depth = tokens.shape
        owned, p_len, _ = store.shape
        hd = w_query.shape[1]
        width = w_pool_in.shape[1]
        tiles = rows // TILE
        half_n = n // 2
        hbm = pl.BlockSpec(memory_space=pl.ANY)
        vmem = pl.BlockSpec(memory_space=pltpu.VMEM)
        smem = pl.BlockSpec(memory_space=pltpu.SMEM)
        dma = pltpu.SemaphoreType.DMA
        return pl.pallas_call(
            functools.partial(kernel, n, tp_size, hd=hd),
            out_shape=jax.ShapeDtypeStruct((rows, width), BF16),
            in_specs=[hbm, smem, hbm, vmem, hbm, hbm, hbm, hbm, smem, hbm, hbm, vmem, vmem],
            out_specs=vmem,
            scratch_shapes=[
                pltpu.VMEM((rows, depth), BF16),
                pltpu.VMEM((owned, p_len, depth), BF16),
                pltpu.VMEM((depth, hd), BF16),
                pltpu.VMEM((depth, hd), BF16),
                pltpu.VMEM((depth, hd), BF16),
                pltpu.VMEM((depth, width), BF16),
                pltpu.VMEM((TILE, depth), BF16),
                pltpu.VMEM((width, width), BF16),
                pltpu.VMEM((tp_size, hd, width), BF16),
                pltpu.VMEM((n, owned, p_len, 2 * hd), BF16),
                pltpu.VMEM((rows, hd), BF16),
                pltpu.VMEM((rows, width), F32),
                pltpu.VMEM((rows, width), F32),
                pltpu.VMEM((rows, hd), F32),
                pltpu.VMEM((rows, p_len), F32),
                pltpu.VMEM((tp_size, rows, hd), BF16),
                dma((6,)),
                dma((tiles,)),
                dma((owned,)),
                dma((3,)),
                dma((3,)),
                dma((2, half_n, owned)),
                dma((2, half_n, owned)),
                dma((3, tiles)),
                dma((3, tiles)),
            ],
            compiler_params=pltpu.CompilerParams(
                collective_id=0,
                has_side_effects=True,
                vmem_limit_bytes=60 * 1024 * 1024,
            ),
        )(
            tokens,
            passage_ids.T,
            store,
            mix_gain,
            w_query,
            w_key,
            w_value,
            w_cross_out,
            head_scale,
            w_pool_in,
            w_pool_mix,
            pool_scale,
            gate_weight.reshape(tp_size, 1, width),
        )

    return jax.shard_map(
        per_device,
        mesh=mesh,
        in_specs=(
            P("st", None),
            P("st", None),
            P("st", None, None),
            P(),
            P(None, "tp"),
            P(None, "tp"),
            P(None, "tp"),
            P("tp", None),
            P(),
            P(None, "tp"),
            P(),
            P(),
            P(),
        ),
        out_specs=P("st", "tp"),
        check_vma=False,
    )
```
